256 devices in a mesh: sp: 64 (over z, x, core), tp: 4 (over y).
Axes of the slice: x: 4, y: 4, z: 8, core: 2. Of those that a mesh axis runs over, the one named last changes fastest.
Arguments:
- queries: bfloat16 [40960, 1024], P('sp', 'tp'), may hold values from -6 to 6
- key_head_rows: bfloat16 [40960, 1024], P('sp', 'tp'), may hold values from -6 to 6
- value_head_rows: bfloat16 [40960, 2048], P('sp', 'tp'), may hold values from -6 to 6
- output_gate_preact: bfloat16 [40960, 2048], P('sp', 'tp'), may hold values from -6 to 6
- log_input_gate: float32 [16, 40960], P('tp', 'sp'), may hold values from -4 to 300
- forget_gate_preact: float32 [16, 40960], P('tp', 'sp')
- extra_log_decay: float32 [16, 40960], P('tp', 'sp'), may hold values from -2.1 to 0
- head_norm_gain: float32 [2048], P('tp'), may hold values from 0.1 to 1.9
- residual: bfloat16 [40960, 2048], P(('sp', 'tp')), may hold values from -6 to 6
- cell_output_weight: bfloat16 [2048, 2048], P('tp'), may hold values from -0.25 to 0.25
- feedforward_norm_gain: float32 [2048], replicated, may hold values from 0.1 to 1.9
- gate_projection_weight: bfloat16 [2048, 5632], P('sp', 'tp'), may hold values from -0.125 to 0.125
- up_projection_weight: bfloat16 [2048, 5632], P('sp', 'tp'), may hold values from -0.125 to 0.125
- down_projection_weight: bfloat16 [5632, 2048], P('tp', 'sp'), may hold values from -0.109375 to 0.109375
Outputs:
- layer_out: bfloat16 [40960, 2048], P(('sp', 'tp'))
The draws below stay inside these ranges and needn't reach their ends.
All inputs are finite; a program needn't handle non-finite values.
Results may differ from the reference program's by a relative error of at most 0.015.
Values may be sent and summed in bfloat16 or wider, within the bound.
A program may use at most 128 MiB of HBM per device.

```python
import jax
import jax.numpy as jnp
from jax import lax

D = 2048
HEADS = 16
DQK = 64
DV = 128
FF = 5632
BLOCK = 128
TOK_DEV = 640
TOKENS = 40960
HV = 2048
N_TP = 4


def draw_log_input_gate(key, part):
    base_key = jax.random.fold_in(key, 0)
    return jnp.clip(jax.random.normal(base_key, (HEADS, TOKENS), jnp.float32), -4.0, 4.0)


def draw_forget_gate_preact(key, part):
    kind_key, block_key, noise_key = jax.random.split(key, 3)
    fast_share = 0.5
    fast_heads = jax.random.uniform(kind_key, (HEADS, 1), jnp.float32) < fast_share
    base_rate = jnp.where(fast_heads, 1.0 / 40.0, 0.5 / TOKENS)
    span_scale = jax.random.uniform(block_key, (HEADS, TOKENS // TOK_DEV), jnp.float32, 0.35, 1.0)
    span_scale = jnp.repeat(span_scale, TOK_DEV, axis=1)
    jitter = jnp.exp(0.7 * jnp.clip(jax.random.normal(noise_key, (HEADS, TOKENS), jnp.float32), -3.0, 3.0))
    decay_rate = base_rate * span_scale * jitter
    return -jnp.log(jnp.expm1(decay_rate))


def draw_extra_log_decay(key, part):
    spot_key, size_key = jax.random.split(key, 2)
    spot_list = jax.random.randint(spot_key, (HEADS, 3), 0, TOKENS)
    drop_sizes = jax.random.uniform(size_key, (HEADS, 3, 1), jnp.float32, 0.22, 0.69)
    hit_mask = jnp.arange(TOKENS)[None, None, :] == spot_list[:, :, None]
    return -jnp.sum(jnp.where(hit_mask, drop_sizes, 0.0), axis=1)


def block_scale(key, shape, shards, least, top_value):
    def one(dim, parts):
        draws = jax.random.uniform(jax.random.fold_in(jax.random.fold_in(key, 6), dim), (parts,), jnp.float32, least / len(shards), top_value / len(shards))
        return jnp.repeat(jnp.exp(draws), shape[dim] // parts).reshape((-1,) + (1,) * (len(shape) - dim - 1))

    factor_of = one(*shards[0])
    for cut in shards[1:]:
        factor_of = factor_of * one(*cut)
    return factor_of


def noise(own_key, shape, scale, most, cuts=(), dtype=jnp.bfloat16):
    result = scale * jax.random.normal(own_key, shape, jnp.float32)
    if cuts:
        result = result * block_scale(own_key, shape, cuts, -0.22, 0.18)
    return jnp.clip(result, -most, most).astype(dtype)


def setup_inputs(seed: int = 0) -> dict:
    key_of = jax.random.split(jax.random.key(seed), 15)
    queries = noise(key_of[0], (TOKENS, HEADS * DQK), 1.0, 6.0, ((0, 64), (1, 4)))
    key_head_rows = noise(key_of[1], (TOKENS, HEADS * DQK), 1.0, 6.0, ((0, 64), (1, 4)))
    value_head_rows = noise(key_of[2], (TOKENS, HV), 1.0, 6.0, ((0, 64), (1, 4)))
    output_gate_preact = noise(key_of[3], (TOKENS, HV), 1.0, 6.0, ((0, 64), (1, 4)))
    log_input_gate = draw_log_input_gate(jax.random.fold_in(key_of[14], 71), 0)
    forget_gate_preact = draw_forget_gate_preact(jax.random.fold_in(key_of[14], 71), 0)
    extra_log_decay = draw_extra_log_decay(jax.random.fold_in(key_of[14], 71), 0)
    head_norm_gain = jnp.clip(1.0 + 0.18 * jax.random.normal(key_of[7], (HV,), jnp.float32), 0.1, 1.9)
    residual = noise(key_of[8], (TOKENS, D), 1.0, 6.0, ((0, 256),))
    cell_output_weight = noise(key_of[9], (HV, D), (HV // 4) ** -0.5, 0.25, ((0, 4),))
    feedforward_norm_gain = jnp.clip(1.0 + 0.18 * jax.random.normal(key_of[10], (D,), jnp.float32), 0.1, 1.9)
    gate_projection_weight = noise(key_of[11], (D, FF), D ** -0.5, 0.125, ((0, 64), (1, 4)))
    up_projection_weight = noise(key_of[12], (D, FF), D ** -0.5, 0.125, ((0, 64), (1, 4)))
    down_projection_weight = noise(key_of[13], (FF, D), (FF // 2) ** -0.5, 0.109375, ((0, 4), (1, 64)))
    return {"queries": queries, "key_head_rows": key_head_rows, "value_head_rows": value_head_rows, "output_gate_preact": output_gate_preact, "log_input_gate": log_input_gate, "forget_gate_preact": forget_gate_preact, "extra_log_decay": extra_log_decay, "head_norm_gain": head_norm_gain, "residual": residual, "cell_output_weight": cell_output_weight, "feedforward_norm_gain": feedforward_norm_gain, "gate_projection_weight": gate_projection_weight, "up_projection_weight": up_projection_weight, "down_projection_weight": down_projection_weight}


epsilon = 1e-06
lowest = -1e+30

def merge_states(earlier, later):
    state_one, top_one, total_one = earlier
    state_two, top_two, total_two = later
    top_new = jnp.maximum(total_two + top_one, top_two)
    scale_one = jnp.exp(total_two + top_one - top_new)
    scale_two = jnp.exp(top_two - top_new)
    state_new = scale_one[..., None, None] * state_one + scale_two[..., None, None] * state_two
    return (state_new, top_new, total_one + total_two)

def block_parts(key_block, value_block, gate_block, forget_block):
    running = jnp.cumsum(forget_block, axis=-1)
    totals = running[..., -1]
    to_end = totals[..., None] - running + gate_block
    top_block = lax.optimization_barrier(jnp.max(to_end, axis=-1))
    factor = jnp.exp(to_end - top_block[..., None]) * DQK ** (-0.5)
    weighted = (key_block.astype(jnp.float32) * factor[..., None]).astype(jnp.bfloat16)
    states = jnp.einsum('nhsd,nhse->nhde', weighted.astype(jnp.float32), value_block.astype(jnp.float32))
    return (running, (states, top_block, totals))

def block_output(query_block, key_block, value_block, gate_block, running, carried_state, carried_top):
    length = query_block.shape[-2]
    scores = jnp.einsum('nhtd,nhsd->nhts', query_block.astype(jnp.float32), key_block.astype(jnp.float32)) * DQK ** (-0.5)
    log_decay = running[..., :, None] - running[..., None, :] + gate_block[..., None, :]
    causal = jnp.arange(length)[:, None] >= jnp.arange(length)[None, :]
    log_decay = jnp.where(causal, log_decay, -jnp.inf)
    carried = running + carried_top[..., None]
    row_top = jnp.maximum(carried, lax.optimization_barrier(jnp.max(log_decay, axis=-1)))
    weights = (scores * jnp.exp(log_decay - row_top[..., None])).astype(jnp.bfloat16)
    within = jnp.einsum('nhts,nhse->nhte', weights.astype(jnp.float32), value_block.astype(jnp.float32))
    across = jnp.einsum('nhtd,nhde->nhte', query_block.astype(jnp.float32), carried_state, precision=lax.Precision.HIGHEST)
    return jnp.exp(carried - row_top)[..., None] * across + within

def grouped_product(left, right, groups):
    columns = left.shape[1] // groups
    summed = jnp.zeros((left.shape[0], right.shape[1]), jnp.float32)
    for member in range(groups):
        product = jnp.dot(left[:, member * columns:(member + 1) * columns], right[member * columns:(member + 1) * columns], preferred_element_type=jnp.float32)
        rounded = lax.optimization_barrier(product.astype(jnp.bfloat16))
        summed = summed + rounded.astype(jnp.float32)
    return summed

def reference(queries, key_head_rows, value_head_rows, output_gate_preact, log_input_gate, forget_gate_preact, extra_log_decay, head_norm_gain, residual, cell_output_weight, feedforward_norm_gain, gate_projection_weight, up_projection_weight, down_projection_weight):
    blocks = TOKENS // BLOCK

    def split_heads(matrix, head_size):
        return matrix.reshape(blocks, BLOCK, HEADS, head_size).transpose(0, 2, 1, 3)

    def split_gate_parts(gates):
        return gates.reshape(HEADS, blocks, BLOCK).transpose(1, 0, 2)
    log_forget_gate = jax.nn.log_sigmoid(forget_gate_preact) + extra_log_decay
    inputs = (split_heads(queries, DQK), split_heads(key_head_rows, DQK), split_heads(value_head_rows, DV), split_gate_parts(log_input_gate), split_gate_parts(log_forget_gate))

    def advance(history, segment):
        query_block, key_block, value_block, gate_block, forget_block = [member[None] for member in segment]
        running, summary = block_parts(key_block, value_block, gate_block, forget_block)
        numerator = block_output(query_block, key_block, value_block, gate_block, running, history[0][None], history[1][None])
        history = merge_states(history, tuple((member[0] for member in summary)))
        return (history, numerator[0])
    initial = (jnp.zeros((HEADS, DQK, DV), jnp.float32), jnp.full((HEADS,), lowest, jnp.float32), jnp.zeros((HEADS,), jnp.float32))
    _, numerators = lax.scan(advance, initial, inputs)
    numerators = numerators.transpose(0, 2, 1, 3).reshape(TOKENS, HEADS, DV)
    normalized = numerators * lax.rsqrt(lax.optimization_barrier(jnp.mean(numerators * numerators, axis=-1, keepdims=True)) + epsilon)
    cell_rows = (normalized.reshape(TOKENS, HV) * head_norm_gain * jax.nn.sigmoid(output_gate_preact.astype(jnp.float32))).astype(jnp.bfloat16)

    def finish(segment):
        cell_block, residual_block = segment
        mixed_rows = (residual_block.astype(jnp.float32) + grouped_product(cell_block, cell_output_weight, N_TP)).astype(jnp.bfloat16)
        mixed_float = mixed_rows.astype(jnp.float32)
        normed = (mixed_float * lax.rsqrt(lax.optimization_barrier(jnp.mean(mixed_float * mixed_float, axis=-1, keepdims=True)) + epsilon) * feedforward_norm_gain).astype(jnp.bfloat16)
        gate_proj = jnp.dot(normed, gate_projection_weight, preferred_element_type=jnp.float32)
        up_proj = jnp.dot(normed, up_projection_weight, preferred_element_type=jnp.float32)
        hidden = (jax.nn.silu(gate_proj) * up_proj).astype(jnp.bfloat16)
        return (mixed_float + grouped_product(hidden, down_projection_weight, N_TP)).astype(jnp.bfloat16)
    outputs = lax.map(finish, (cell_rows.reshape(TOKENS // TOK_DEV, TOK_DEV, HV), residual.reshape(TOKENS // TOK_DEV, TOK_DEV, D)))
    return outputs.reshape(TOKENS, D)
```

```python
import jax
import jax.numpy as jnp
from jax import lax
from jax.experimental import pallas as pl
from jax.experimental.pallas import tpu as pltpu
from jax.sharding import Mesh
from jax.sharding import PartitionSpec as P

BF = jnp.bfloat16
F32 = jnp.float32
DQK = 64
BLOCK = 128
NZ, NX, NC, NY = 8, 4, 2, 4
ROWS = 640
NB = 5
MINE = 160
D = 2048
FFL = 1408
SHARD = 32
MSG = 160
EPS = 1e-6
LOWEST = -1e30
MESH = pl.DeviceIdType.MESH
SP = ("z", "x", "c")
SP_TP = ("z", "x", "c", "y")


def nt_dot(a, b):
    return lax.dot_general(a, b, (((1,), (1,)), ((), ())), preferred_element_type=F32)


def tn_dot(a, b):
    return lax.dot_general(a, b, (((0,), (0,)), ((), ())), preferred_element_type=F32)


def dot(a, b):
    return jnp.dot(a, b, preferred_element_type=F32)


def lane_scan(x, op, blank):
    lane = lax.broadcasted_iota(jnp.int32, x.shape, 1)
    for k in (1, 2, 4, 8, 16, 32, 64):
        x = op(x, jnp.where(lane >= k, pltpu.roll(x, k, 1), blank))
    return x


def expand(e, r):
    return jnp.concatenate(
        [
            jnp.broadcast_to(e[r : r + 1, :], (64, 128)),
            jnp.broadcast_to(e[r + 1 : r + 2, :], (64, 128)),
        ],
        axis=0,
    )


def merge(one, two):
    s1, t1, a1 = one
    s2, t2, a2 = two
    top = jnp.maximum(a2 + t1, t2)
    e1 = jnp.exp(a2 + t1 - top)
    e2 = jnp.exp(t2 - top)
    return expand(e1, 0) * s1 + expand(e2, 0) * s2, top, a1 + a2


def pack(ref, at, parts):
    s, top, tot = parts
    row = lax.broadcasted_iota(jnp.int32, (8, 128), 0)
    t = jnp.where(row < 4, top, pltpu.roll(tot, 4, 0))
    hi = t.astype(BF).astype(F32)
    rest = t - hi
    mid = rest.astype(BF).astype(F32)
    low = rest - mid
    ref[at, 0:128, :] = s.astype(BF)
    ref[at, 128:160, :] = jnp.concatenate([hi, mid, low, jnp.zeros_like(t)], axis=0).astype(BF)


def unpack(ref, at):
    s = ref[at, 0:128, :].astype(F32)
    m = ref[at, 128:160, :].astype(F32)
    t = m[0:8] + m[8:16] + m[16:24]
    return s, t, pltpu.roll(t, 4, 0)


def blank_parts():
    return (
        jnp.zeros((128, 128), F32),
        jnp.full((8, 128), LOWEST, F32),
        jnp.zeros((8, 128), F32),
    )


def kernel(
    q_h, k_h, v_h, o_h, ig_h, fg_h, ed_h, hg_h, res_h, wo_h, ng_h, wg_h, wu_h, wd_h,
    out_h,
    q_v, k_v, v_v, o_v, ig_v, fg_v, ed_v, hg_v, res_v, ng_v,
    wgu, wdn, wdt, wo, xs, hid, part, rfar, rnear, crows, relay, cell, num, mix, out_v,
    ltop_s, ltot_s, a_s, ml_s, fac_s, e1_s, e2_s, e1c, e2c, acc, lst, lpre, sm1, cb, xb, zb, st2, inb,
    lsem, ssem, rsem,
):
    z, x, c, y = (lax.axis_index(n) for n in ("z", "x", "c", "y"))

    def zz(d):
        return lax.rem(z + (d + NZ), NZ)

    def xx(d):
        return lax.rem(x + (d + NX), NX)

    def yy(d):
        return lax.rem(y + (d + NY), NY)

    oc = 1 - c

    local = {}

    def load(name, src, dst):
        cp = pltpu.make_async_copy(src, dst, lsem.at[len(local)])
        cp.start()
        local[name] = cp

    load("wg", wg_h, wgu.at[z, x, c, :, pl.ds(0, FFL)])
    load("wu", wu_h, wgu.at[z, x, c, :, pl.ds(FFL, FFL)])
    load("wd", wd_h, wdn.at[z, x, c])
    load("wo", wo_h, wo.at[y])
    load("fg", fg_h, fg_v)
    load("ed", ed_h, ed_v)
    load("ig", ig_h, ig_v)
    load("k", k_h, k_v)
    load("v", v_h, v_v)
    load("q", q_h, q_v)
    load("o", o_h, o_v)
    load("hg", hg_h, hg_v)
    load("res", res_h, res_v)
    load("ng", ng_h, ng_v)

    bar = pltpu.get_barrier_semaphore()
    pals = (
        [{"z": zz(d)} for d in range(1, NZ)]
        + [{"x": xx(d)} for d in range(1, NX)]
        + [{"y": yy(d)} for d in range(1, NY)]
        + [{"c": oc}]
    )
    for pal in pals:
        pl.semaphore_signal(bar, inc=1, device_id=pal, device_id_type=MESH)
    with jax.named_scope("barrier"):
        pl.semaphore_wait(bar, len(pals))

    numbers = {}
    leaving = {}

    def number(key):
        return numbers.setdefault(key, len(numbers))

    def copy(src, dst, n_send, n_recv, dev):
        return pltpu.make_async_remote_copy(
            src_ref=src, dst_ref=dst, send_sem=ssem.at[n_send], recv_sem=rsem.at[n_recv],
            device_id=dev, device_id_type=MESH,
        )

    def send(out, key, src, dst, dev):
        n = leaving.setdefault(out, len(leaving))
        copy(src, dst, n, number(key), dev).start()

    def recv(key, land):
        copy(land, land, 0, number(key), partner).wait_recv()

    def drain(out, like):
        copy(like, like, leaving[out], 0, partner).wait_send()

    right_z, left_z = {"z": zz(1)}, {"z": zz(-1)}
    right_x, left_x = {"x": xx(1)}, {"x": xx(-1)}
    right_y, left_y = {"y": yy(1)}, {"y": yy(-1)}
    partner = {"c": oc}

    def gu(zb, xb, which=None):
        if which is None:
            return wgu.at[zb, xb, c]
        return wgu.at[zb, xb, c, :, pl.ds(which * FFL, FFL)]

    def dn_half(h):
        return pl.ds(0, 768) if h == 0 else pl.ds(768, 640)

    def dnx(xb, h=None):
        if h is None:
            return wdn.at[z, xb, c]
        return wdn.at[z, xb, c, :, dn_half(h)]

    def dnz(zb, h=None):
        if h is None:
            return wdn.at[zb, :, c]
        return wdn.at[zb, :, c, :, dn_half(h)]

    def bz_send(s):
        w0, w1 = (None, None) if s < 4 else (0, 1)
        out = "bz" if s < 4 else "hz"
        send(out, ("bz", s), gu(zz(1 - s), x, w0), gu(zz(1 - s), x, w0), right_z)
        send(out, ("bz", s), gu(zz(s - 1), x, w1), gu(zz(s - 1), x, w1), left_z)

    def bz_recv(s):
        recv(("bz", s), wgu.at[z, 0] if s < 4 else gu(zz(4), x))

    def bz_step(s):
        bz_recv(s)
        if s < 4:
            bz_send(s + 1)

    def bx_send(o):
        send("bx", ("bx", o), gu(zz(o), x), gu(zz(o), x), right_x)
        send("bx", ("bx", o), gu(zz(o), x), gu(zz(o), x), left_x)

    def bx_mid(o):
        recv(("bx", o), wgu.at[zz(o), 0])
        send("hx", ("hx", o), gu(zz(o), xx(-1), 0), gu(zz(o), xx(-1), 0), right_x)
        send("hx", ("hx", o), gu(zz(o), xx(1), 1), gu(zz(o), xx(1), 1), left_x)

    def bx_fin(o):
        recv(("hx", o), gu(zz(o), xx(2)))
        send("db", "db", wgu.at[zz(o), :, c], wgu.at[zz(o), :, c], partner)

    def db_recv():
        recv("db", wgu.at[0:4])

    def ax_send():
        send("hz", "ax", dnx(x), dnx(x), right_x)
        send("hz", "ax", dnx(x), dnx(x), left_x)

    def ax_mid():
        recv("ax", wdn.at[z, 0])
        send("ax", "hax", dnx(xx(-1), 0), dnx(xx(-1), 0), right_x)
        send("ax", "hax", dnx(xx(1), 1), dnx(xx(1), 1), left_x)

    def ax_fin():
        recv("hax", dnx(xx(2)))

    def az_send(s):
        w0, w1 = (None, None) if s < 4 else (0, 1)
        out = "az" if s < 4 else "haz"
        send(out, ("az", s), dnz(zz(1 - s), w0), dnz(zz(1 - s), w0), right_z)
        send(out, ("az", s), dnz(zz(s - 1), w1), dnz(zz(s - 1), w1), left_z)

    def da_send(o):
        send("da", ("da", o), wdn.at[zz(o), :, c], wdn.at[zz(o), :, c], partner)

    def turn(o):
        recv(("da", o), wdn.at[zz(o), :, oc])
        cols = pl.ds(pl.multiple_of(256 * zz(o), 256), 256)

        @pl.loop(0, FFL // 128)
        def _(n):
            rows = pl.ds(pl.multiple_of(n * 128, 128), 128)
            wdt[rows, cols] = wdn[zz(o), :, :, :, rows].reshape(256, 128).T

    def az_step(s):
        recv(("az", s), wdn.at[z] if s < 4 else dnz(zz(4)))
        if s < 4:
            az_send(s + 1)
            da_send(-s)
            da_send(s)
        else:
            da_send(4)

    def wo_half(yb, cc):
        return wo.at[yb, pl.ds(pl.multiple_of(256 * cc, 256), 256)]

    def wo_piece(yb, cc, k):
        return wo.at[yb, pl.ds(pl.multiple_of(256 * cc + 64 * k, 64), 64)]

    def wo_send():
        send("wo", "wo", wo_half(y, c), wo_half(y, c), right_y)
        send("wo", "wo", wo_half(y, c), wo_half(y, c), left_y)

    def wo_mid():
        recv("wo", wo.at[y])
        for k in (0, 1):
            send("fwo", ("fwo", k), wo_piece(yy(-1), c, k), wo_piece(yy(-1), c, k), right_y)
            send("fwo", ("fwo", k), wo_piece(yy(1), c, 2 + k), wo_piece(yy(1), c, 2 + k), left_y)
        send("dwo", "dwo", wo_half(yy(-1), c), wo_half(yy(-1), c), partner)
        send("dwo", "dwo", wo_half(yy(1), c), wo_half(yy(1), c), partner)

    def wo_fin():
        for k in (0, 1):
            recv(("fwo", k), wo.at[yy(2), 0:128])
            for h in (k, 2 + k):
                send("dfwo", "dfwo", wo_piece(yy(2), c, h), wo_piece(yy(2), c, h), partner)

    local["wg"].wait()
    local["wu"].wait()
    bz_send(1)
    bx_send(0)
    local["wo"].wait()
    wo_send()

    for name in ("fg", "ed", "ig", "k", "v"):
        local[name].wait()
    lane = lax.broadcasted_iota(jnp.int32, (128, 128), 1)
    subl = lax.broadcasted_iota(jnp.int32, (128, 128), 0)
    row8 = lax.broadcasted_iota(jnp.int32, (8, 128), 0)
    low = lane < 64
    causal = subl >= lane

    def by_block(ref):
        return jnp.concatenate(
            [ref[:, 128 * b : 128 * b + 128] for b in range(NB) for _ in (0, 1)], axis=0
        )

    with jax.named_scope("gates"):
        fg, ig, ed = by_block(fg_v), by_block(ig_v), by_block(ed_v)
        wide = (8 * NB, 128)
        lf = jnp.minimum(fg, 0.0) - jnp.log1p(jnp.exp(-jnp.abs(fg))) + ed
        run = lane_scan(lf, jnp.add, 0.0)
        last = lax.broadcasted_iota(jnp.int32, wide, 1) == 127
        tot = jnp.broadcast_to(jnp.sum(jnp.where(last, run, 0.0), axis=1, keepdims=True), wide)
        a = ig - run
        te = tot - run + ig
        bt = jnp.broadcast_to(jnp.max(te, axis=1, keepdims=True), wide)
        fac = jnp.exp(te - bt) * DQK ** (-0.5)
        cm = lane_scan(a, jnp.maximum, -3e38)
        ltop, ltot = jnp.full((8, 128), LOWEST, F32), jnp.zeros((8, 128), F32)
        for b in range(NB):
            at = slice(8 * b, 8 * b + 8)
            ltop_s[b], ltot_s[b] = ltop, ltot
            a_s[b] = a[at]
            ml_s[b] = jnp.maximum(ltop, cm[at])
            fac_s[b] = fac[at]
            top = jnp.maximum(tot[at] + ltop, bt[at])
            e1_s[b] = jnp.exp(tot[at] + ltop - top)
            e2_s[b] = jnp.exp(bt[at] - top)
            ltop, ltot = top, ltot + tot[at]
    lst[...] = jnp.zeros((2, 128, 128), F32)

    with jax.named_scope("states"):
        @pl.loop(0, NB)
        def _(b):
            rows = pl.ds(pl.multiple_of(b * 128, 128), 128)
            fact = fac_s[b].T
            e1, e2 = e1_s[b], e2_s[b]
            for p in (0, 1):
                f2 = jnp.where(low, fact[:, 2 * p : 2 * p + 1], fact[:, 2 * p + 1 : 2 * p + 2])
                wk = (k_v[rows, 128 * p : 128 * p + 128].astype(F32) * f2).astype(BF)
                s2 = tn_dot(wk, v_v[rows, 256 * p : 256 * p + 256])
                sb = jnp.concatenate([s2[0:64, 0:128], s2[64:128, 128:256]], axis=0)
                old = lst[p]
                lpre[b, p] = old.astype(BF)
                lst[p] = expand(e1, 2 * p) * old + expand(e2, 2 * p) * sb

    pack(sm1, 0, (lst[0], ltop, ltot))
    pack(sm1, 1, (lst[1], pltpu.roll(ltop, 6, 0), pltpu.roll(ltot, 6, 0)))
    send("sc", "sc1", sm1.at[oc], cb.at[c], partner)
    cb[c] = sm1[c]

    def inner(b):
        rows = pl.ds(pl.multiple_of(b * 128, 128), 128)
        a, ml = a_s[b], ml_s[b]
        mc = ml.T
        ec = jnp.exp(ltop_s[b] - ml).T
        for p in (0, 1):
            qp = q_v[rows, 128 * p : 128 * p + 128]
            kp = k_v[rows, 128 * p : 128 * p + 128]
            lp = lpre[b, p]
            for e in (0, 1):
                h = 2 * p + e
                qm = jnp.where(low if e == 0 else jnp.logical_not(low), qp, jnp.zeros_like(qp))
                s = nt_dot(qm, kp) * DQK ** (-0.5)
                w = jnp.exp(jnp.where(causal, a[h : h + 1, :] - mc[:, h : h + 1], LOWEST))
                w = (s * w).astype(BF)
                hs = pl.ds(128 * h, 128)
                num[rows, hs] = dot(w, v_v[rows, hs]) + ec[:, h : h + 1] * dot(qm, lp)

    local["q"].wait()
    with jax.named_scope("sc1"):
        recv("sc1", cb.at[oc])
    core0 = unpack(cb, 0)
    pack(xb, x, merge(core0, unpack(cb, 1)))
    for d in (1, 3, 2):
        send("sx", "sx", xb.at[x], xb.at[x], {"x": xx(d)})
    local["wd"].wait()
    ax_send()
    with jax.named_scope("bz1"):
        bz_step(1)
    bx_send(-1)
    bx_send(1)

    with jax.named_scope("inner"):
        @pl.loop(0, NB)
        def _(b):
            inner(b)

    with jax.named_scope("sx"):
        recv("sx", xb.at[0:3])

    def into(ref):
        return lambda k, acc: merge(acc, unpack(ref, k))

    with jax.named_scope("sxmerge"):
        xpre = lax.fori_loop(0, x, into(xb), blank_parts())
        pack(zb, z, lax.fori_loop(x, NX, into(xb), xpre))
    for d in (1, 7, 2, 6, 3, 5, 4):
        send("sz", "sz", zb.at[z], zb.at[z], {"z": zz(d)})
    with jax.named_scope("bxm0"):
        bx_mid(0)
    with jax.named_scope("axm"):
        ax_mid()
    with jax.named_scope("bz2"):
        bz_step(2)
    bx_send(-2)
    bx_send(2)
    with jax.named_scope("sz"):
        recv("sz", zb.at[0:7])
    with jax.named_scope("szmerge"):
        zpre = lax.fori_loop(0, z, into(zb), blank_parts())
        in0 = merge(zpre, xpre)
        pack(st2, 0, in0)
        pack(st2, 1, merge(in0, core0))
    send("sc", "sc2", st2.at[oc], inb.at[c], partner)
    inb[c] = st2[c]
    with jax.named_scope("axf"):
        ax_fin()
    az_send(1)
    da_send(0)

    local["o"].wait()
    local["hg"].wait()
    with jax.named_scope("sc2"):
        recv("sc2", inb.at[oc])
    ta = unpack(inb, 0)[1]
    tb = unpack(inb, 1)[1]
    top_in = jnp.where(row8 < 2, ta, pltpu.roll(tb, 2, 0))

    with jax.named_scope("ecol"):
        for b in range(NB):
            ml = ml_s[b]
            g = ltot_s[b] + top_in
            m = jnp.maximum(ml, g)
            rows = pl.ds(128 * b, 128)
            e1c[rows, :] = jnp.exp(ml - m).T
            e2c[rows, :] = jnp.exp(g - m).T

    low160 = lax.broadcasted_iota(jnp.int32, (MINE, 128), 1) < 64

    def rows_of(d):
        return pl.ds(pl.multiple_of(MINE * yy(d), 32), MINE)

    def finish(d):
        rows = rows_of(d)
        e1, e2 = e1c[rows, :], e2c[rows, :]
        for p in (0, 1):
            qp = q_v[rows, 128 * p : 128 * p + 128]
            sin = inb[p, 0:128, :]
            for e in (0, 1):
                h = 2 * p + e
                hs = pl.ds(128 * h, 128)
                qm = jnp.where(low160 if e == 0 else jnp.logical_not(low160), qp, jnp.zeros_like(qp))
                n = e1[:, h : h + 1] * num[rows, hs] + e2[:, h : h + 1] * dot(qm, sin)
                r = lax.rsqrt(jnp.mean(n * n, axis=1, keepdims=True) + EPS)
                gate = 1.0 / (1.0 + jnp.exp(-o_v[rows, hs].astype(F32)))
                cell[rows, hs] = (n * r * hg_v[:, hs] * gate).astype(BF)

    ha, hb = pl.ds(0, 80), pl.ds(80, 80)

    def half_of(d, h):
        return pl.ds(pl.multiple_of(MINE * yy(d) + 80 * h, 16), 80)

    with jax.named_scope("finish"):
        finish(2)
        send("caf", "caf", cell.at[half_of(2, 0)], relay.at[0], right_y)
        send("caf", "caf", cell.at[half_of(2, 1)], relay.at[1], left_y)
        finish(1)
        send("ca", "ca", cell.at[rows_of(1)], crows.at[1], right_y)
        finish(3)
        send("ca", "ca", cell.at[rows_of(3)], crows.at[3], left_y)
    with jax.named_scope("wo_mid"):
        wo_mid()
    with jax.named_scope("finish0"):
        finish(0)
    with jax.named_scope("bxm1"):
        bx_mid(-1)
        bx_mid(1)
    with jax.named_scope("bz3"):
        bz_step(3)
    bx_send(-3)
    bx_send(3)

    local["res"].wait()
    local["ng"].wait()

    def project(lhs, yb, first):
        @pl.loop(0, 4, unroll=True)
        def _(n):
            cols = pl.ds(pl.multiple_of(n * 512, 512), 512)
            old = res_v[:, cols].astype(F32) if first else acc[:, cols]
            acc[:, cols] = old + dot(lhs(), wo[yb, :, cols])

    with jax.named_scope("proj0"):
        project(lambda: cell[rows_of(0), :], y, True)
    with jax.named_scope("caf"):
        recv("caf", relay)
        send("cag", "cag", relay.at[0], crows.at[2, ha], right_y)
        send("cag", "cag", relay.at[1], crows.at[2, hb], left_y)
    with jax.named_scope("bxf0"):
        bx_fin(0)

    with jax.named_scope("az1"):
        az_step(1)
    with jax.named_scope("ca"):
        recv("ca", crows.at[0:2])
    with jax.named_scope("dwo"):
        recv("dwo", wo.at[y])
    with jax.named_scope("projnear"):
        project(lambda: crows[1], yy(-1), False)
        project(lambda: crows[3], yy(1), False)
    with jax.named_scope("bxm2"):
        bx_mid(-2)
        bx_mid(2)
    with jax.named_scope("bz4"):
        bz_recv(4)
    bx_send(4)
    with jax.named_scope("bxf1"):
        bx_fin(-1)
        bx_fin(1)
    with jax.named_scope("bxm3"):
        bx_mid(-3)
        bx_mid(3)
    with jax.named_scope("az2"):
        az_step(2)
    with jax.named_scope("wo_fin"):
        wo_fin()
    with jax.named_scope("cag"):
        recv("cag", crows.at[2])
    with jax.named_scope("dwofar"):
        recv("dfwo", wo.at[yy(2), 0:256])
    with jax.named_scope("projfar"):
        project(lambda: crows[2], yy(2), False)

    def norm_rows(first, count):
        @pl.loop(0, count // 16)
        def _(r):
            rows = pl.ds(pl.multiple_of(first + r * 16, 16), 16)
            mb = acc[rows, :].astype(BF)
            mix[rows, :] = mb
            m = mb.astype(F32)
            scale = lax.rsqrt(jnp.mean(m * m, axis=1, keepdims=True) + EPS)
            xs[first // 80, pl.ds(pl.multiple_of(r * 16, 16), 16), :] = (m * scale * ng_v[...]).astype(BF)

    with jax.named_scope("norm"):
        norm_rows(0, 80)
        send("x", "xfirst", xs.at[0], xs.at[2], right_y)
        norm_rows(80, 80)
        send("x", "xfirst", xs.at[1], xs.at[3], left_y)
        send("x", "xsecond", xs.at[1], xs.at[4], right_y)
        send("x", "xsecond", xs.at[0], xs.at[5], left_y)

    with jax.named_scope("bxf2"):
        bx_fin(-2)
        bx_fin(2)
    with jax.named_scope("bxm4"):
        bx_mid(4)
    with jax.named_scope("bxf3"):
        bx_fin(-3)
        bx_fin(3)
    with jax.named_scope("az3"):
        az_step(3)
    with jax.named_scope("turn0"):
        for o in (0, -1, 1):
            turn(o)
    with jax.named_scope("xfwd"):
        recv("xfirst", xs.at[2:4])
        send("xf", "xfar", xs.at[2], xs.at[6], right_y)
        send("xf", "xfar", xs.at[3], xs.at[7], left_y)
    with jax.named_scope("bxf4"):
        bx_fin(4)
    with jax.named_scope("az4"):
        az_step(4)
    with jax.named_scope("turn1"):
        for o in (-2, 2):
            turn(o)
    with jax.named_scope("db"):
        db_recv()

    def up(first, count, fast=True):
        @pl.loop(0, FFL // 128, unroll=fast)
        def _(n):
            gc = pl.ds(pl.multiple_of(n * 128, 128), 128)
            uc = pl.ds(pl.multiple_of(FFL + n * 128, 128), 128)
            w = jnp.concatenate(
                [wgu[:, :, :, :, gc].reshape(D, 128), wgu[:, :, :, :, uc].reshape(D, 128)], axis=1
            )
            r = dot(xs[first : first + count].reshape(count * 80, D), w)
            g, u = r[:, :128], r[:, 128:]
            h = g / (1.0 + jnp.exp(-g)) * u
            hid[80 * first : 80 * (first + count), gc] = h.astype(BF)

    def down(slots, lo, hi, fast=True):
        first, count = slots

        @pl.loop(lo, hi, unroll=fast)
        def _(n):
            cols = pl.ds(pl.multiple_of(n * 256, 256), 256)
            r = dot(hid[80 * first : 80 * (first + count), :], wdt[:, cols])
            part[first : first + count, :, cols] = r.astype(BF).reshape(count, 80, 256)

    lh, rh = pl.ds(0, 1024), pl.ds(1024, 1024)
    with jax.named_scope("upfirst"):
        up(2, 2)
    with jax.named_scope("turn2"):
        for o in (-3, 3, 4):
            turn(o)
    with jax.named_scope("dnfirst"):
        down((2, 1), 0, 4)
        down((3, 1), 4, 8)
    with jax.named_scope("xsecond"):
        recv("xsecond", xs.at[4:6])
    with jax.named_scope("upsecond"):
        up(4, 2)
    with jax.named_scope("dnsecond"):
        down((4, 1), 0, 4)
        for k, s in enumerate((2, 4)):
            send("rn", "rn", part.at[s, :, lh], rnear.at[1, k, :, lh], left_y)
        down((5, 1), 4, 8)
        for k, s in enumerate((5, 3)):
            send("rn", "rn", part.at[s, :, rh], rnear.at[0, k, :, rh], right_y)
    with jax.named_scope("xfar"):
        recv("xfar", xs.at[6:8])
    with jax.named_scope("upfar"):
        up(6, 2)
    with jax.named_scope("dnfar"):
        down((6, 2), 0, 4)
        for k in (0, 1):
            send("rf", ("rf", k), part.at[6 + k, :, lh], rfar.at[0, k], right_y)
        down((6, 2), 4, 8)
        for k in (0, 1):
            send("rf", ("rf", k), part.at[6 + k, :, rh], rfar.at[1, k], left_y)
    with jax.named_scope("dnnear2"):
        down((5, 1), 0, 4)
        down((3, 1), 0, 4)
        down((2, 1), 4, 8)
        down((4, 1), 4, 8)
    with jax.named_scope("upown"):
        up(0, 2, False)

    def add_into(slot, half, side, k):
        @pl.loop(0, 5)
        def _(r):
            rows = pl.ds(pl.multiple_of(r * 16, 16), 16)
            part[slot, rows, half] = (
                part[slot, rows, half].astype(F32) + rfar[side, k, rows, :].astype(F32)
            ).astype(BF)

    for k in (0, 1):
        with jax.named_scope("rf%d" % k):
            recv(("rf", k), rfar.at[0])
        after, before = (5, 3)[k], (2, 4)[k]
        add_into(after, lh, 0, k)
        send("rg", ("rg", k), part.at[after, :, lh], rnear.at[0, k, :, lh], right_y)
        add_into(before, rh, 1, k)
        send("rg", ("rg", k), part.at[before, :, rh], rnear.at[1, k, :, rh], left_y)
    with jax.named_scope("dnown"):
        down((0, 2), 0, 8, False)
    with jax.named_scope("drain"):
        drain("bz", wgu.at[0, 0:3])
        drain("bx", wgu.at[0:2])
        drain("hx", wdn.at[0:2])
        drain("hz", wdn.at[0, 0:2])
        drain("ax", wdn.at[0, 0, 0])
        drain("az", wdn.at[0:3])
        drain("haz", wdn.at[0, 0:2])
        drain("db", wgu.at[0:4])
        drain("da", wdn.at[0:4])
        drain("wo", wo.at[0])
        drain("fwo", wo.at[0, 0:256])
        drain("dwo", wo.at[0])
        drain("dfwo", wo.at[0, 0:256])
        drain("sc", st2)
        drain("sx", xb.at[0:3])
        drain("sz", zb.at[0:7])
        drain("ca", crows.at[0:2])
        drain("caf", relay)
        drain("cag", relay)
        drain("x", xs.at[0:4])
        drain("xf", xs.at[0:2])
        drain("rn", rfar)
        drain("rf", rfar)

    with jax.named_scope("rn"):
        recv("rn", rfar)
    for k in (0, 1):
        with jax.named_scope("rg%d" % k):
            recv(("rg", k), rfar.at[0])

        @pl.loop(0, 5)
        def _(r):
            rows = pl.ds(pl.multiple_of(r * 16, 16), 16)
            all_rows = pl.ds(pl.multiple_of(80 * k + r * 16, 16), 16)
            t = part[k, rows, :].astype(F32) + rnear[0, k, rows, :].astype(F32)
            t = t + rnear[1, k, rows, :].astype(F32)
            out_v[all_rows, :] = (mix[all_rows, :].astype(F32) + t).astype(BF)

        if k == 0:
            early = pltpu.make_async_copy(out_v.at[ha], out_h.at[ha], lsem.at[0])
            early.start()

    done = pltpu.make_async_copy(out_v.at[hb], out_h.at[hb], lsem.at[1])
    done.start()
    drain("rg", rfar)
    early.wait()
    done.wait()


def per_device(q, k, v, o, ig, fg, ed, hg, res, wo, ng, wg, wu, wd):
    hbm = pl.BlockSpec(memory_space=pltpu.HBM)
    vm = pltpu.VMEM
    scratch = [
        vm((ROWS, 256), BF), vm((ROWS, 256), BF), vm((ROWS, 512), BF), vm((ROWS, 512), BF),
        vm((4, ROWS), F32), vm((4, ROWS), F32), vm((4, ROWS), F32),
        vm((1, 512), F32), vm((MINE, D), BF), vm((1, D), F32),
        vm((NZ, NX, NC, SHARD, 2 * FFL), BF), vm((NZ, NX, NC, SHARD, FFL), BF),
        vm((FFL, D), BF),
        vm((NY, 512, D), BF), vm((8, 80, D), BF), vm((ROWS, FFL), BF),
        vm((8, 80, D), BF), vm((2, 2, 80, 1024), BF), vm((2, 2, 80, D), BF),
        vm((NY, MINE, 512), BF), vm((2, 80, 512), BF), vm((ROWS, 512), BF), vm((ROWS, 512), F32),
        vm((MINE, D), BF), vm((MINE, D), BF),
        vm((NB, 8, 128), F32), vm((NB, 8, 128), F32), vm((NB, 8, 128), F32), vm((NB, 8, 128), F32),
        vm((NB, 8, 128), F32), vm((NB, 8, 128), F32), vm((NB, 8, 128), F32),
        vm((ROWS, 8), F32), vm((ROWS, 8), F32), vm((MINE, D), F32),
        vm((2, 128, 128), F32), vm((NB, 2, 128, 128), BF),
        vm((2, MSG, 128), BF), vm((2, MSG, 128), BF), vm((NX, MSG, 128), BF),
        vm((NZ, MSG, 128), BF), vm((2, MSG, 128), BF), vm((2, MSG, 128), BF),
        pltpu.SemaphoreType.DMA((14,)),
        pltpu.SemaphoreType.DMA((24,)),
        pltpu.SemaphoreType.DMA((55,)),
    ]
    return pl.pallas_call(
        kernel,
        out_shape=jax.ShapeDtypeStruct((MINE, D), BF),
        in_specs=[hbm] * 14,
        out_specs=hbm,
        scratch_shapes=scratch,
        compiler_params=pltpu.CompilerParams(
            collective_id=0, has_side_effects=True, vmem_limit_bytes=60 * 1024 * 1024
        ),
        name="cell_ffn",
    )(q, k, v, o, ig, fg, ed, hg.reshape(1, 512), res, wo, ng.reshape(1, D), wg, wu, wd.T)


def solution(mesh):
    torus = Mesh(mesh.devices.reshape(NZ, NX, NC, NY), SP_TP)
    placed = (
        P(SP, "y"), P(SP, "y"), P(SP, "y"), P(SP, "y"),
        P("y", SP), P("y", SP), P("y", SP),
        P("y"), P(SP_TP, None), P("y", None), P(),
        P(SP, "y"), P(SP, "y"), P("y", SP),
    )
    return jax.shard_map(
        per_device, mesh=torus, in_specs=placed, out_specs=P(SP_TP, None), check_vma=False
    )
```

```python
import jax
import jax.numpy as jnp
from jax import lax
from jax.experimental import pallas as pl
from jax.experimental.pallas import tpu as pltpu
from jax.sharding import Mesh
from jax.sharding import PartitionSpec as P

BF = jnp.bfloat16
F32 = jnp.float32
DQK = 64
BLOCK = 128
NZ, NX, NC, NY = 8, 4, 2, 4
ROWS = 640
NB = 5
MINE = 160
D = 2048
FFL = 1408
SHARD = 32
CL = 1280
CA, CB = 384, 384
CR = CA + CB
MSG = 144
EPS = 1e-6
LOWEST = -1e30
MESH = pl.DeviceIdType.MESH
SP = ("z", "x", "c")
SP_TP = ("z", "x", "c", "y")


def nt_dot(a, b):
    return lax.dot_general(a, b, (((1,), (1,)), ((), ())), preferred_element_type=F32)


def tn_dot(a, b):
    return lax.dot_general(a, b, (((0,), (0,)), ((), ())), preferred_element_type=F32)


def dot(a, b):
    return jnp.dot(a, b, preferred_element_type=F32)


def lane_scan(x, op, blank):
    lane = lax.broadcasted_iota(jnp.int32, x.shape, 1)
    for k in (1, 2, 4, 8, 16, 32, 64):
        x = op(x, jnp.where(lane >= k, pltpu.roll(x, k, 1), blank))
    return x


def expand(e, r):
    return jnp.concatenate(
        [
            jnp.broadcast_to(e[r : r + 1, :], (64, 128)),
            jnp.broadcast_to(e[r + 1 : r + 2, :], (64, 128)),
        ],
        axis=0,
    )


def merge(one, two):
    s1, t1, a1 = one
    s2, t2, a2 = two
    top = jnp.maximum(a2 + t1, t2)
    e1 = jnp.exp(a2 + t1 - top)
    e2 = jnp.exp(t2 - top)
    return expand(e1, 0) * s1 + expand(e2, 0) * s2, top, a1 + a2


def pack(ref, at, parts):
    s, top, tot = parts
    row = lax.broadcasted_iota(jnp.int32, (8, 128), 0)
    t = jnp.where(row < 4, top, pltpu.roll(tot, 4, 0))
    hi = t.astype(BF).astype(F32)
    rest = t - hi
    mid = rest.astype(BF).astype(F32)
    low = rest - mid
    ref[at, 0:128, :] = s.astype(BF)
    upper = jnp.where((row & 3) < 2, hi, pltpu.roll(low, 2, 0))
    ref[at, 128:144, :] = jnp.concatenate([upper, mid], axis=0).astype(BF)


def unpack(ref, at):
    s = ref[at, 0:128, :].astype(F32)
    m = ref[at, 128:144, :].astype(F32)
    t = m[0:8] + m[8:16] + pltpu.roll(m[0:8], 6, 0)
    return s, t, pltpu.roll(t, 4, 0)


def blank_parts():
    return (
        jnp.zeros((128, 128), F32),
        jnp.full((8, 128), LOWEST, F32),
        jnp.zeros((8, 128), F32),
    )


def kernel(
    q_h, k_h, v_h, o_h, ig_h, fg_h, ed_h, hg_h, res_h, wo_h, ng_h, wg_h, wu_h, wd_h,
    out_h,
    q_v, k_v, v_v, o_v, ig_v, fg_v, ed_v, hg_v, res_v, ng_v,
    wgu, wdn, wdt, begun, wo, xs, hid, part, rfar, rnear, crows, relay, po, ofa, ofb, on, cell, num, mix, out_v,
    ltop_s, ltot_s, a_s, ml_s, fac_s, e1_s, e2_s, e1c, e2c, acc, lst, lpre, sm1, cb, xb, zb, st2, inb,
    lsem, ssem, rsem,
):
    z, x, c, y = (lax.axis_index(n) for n in ("z", "x", "c", "y"))

    def zz(d):
        return lax.rem(z + (d + NZ), NZ)

    def xx(d):
        return lax.rem(x + (d + NX), NX)

    def yy(d):
        return lax.rem(y + (d + NY), NY)

    oc = 1 - c

    local = {}

    def load(name, src, dst):
        cp = pltpu.make_async_copy(src, dst, lsem.at[len(local)])
        cp.start()
        local[name] = cp

    load("wg", wg_h, wgu.at[z, x, c, :, pl.ds(0, FFL)])
    load("wu", wu_h, wgu.at[z, x, c, :, pl.ds(FFL, FFL)])
    load("wd", wd_h, wdn.at[z, x, c])
    load("wo", wo_h, wo.at[y])
    load("fg", fg_h, fg_v)
    load("ed", ed_h, ed_v)
    load("ig", ig_h, ig_v)
    load("k", k_h, k_v)
    load("v", v_h, v_v)
    load("q", q_h, q_v)
    load("o", o_h, o_v)
    load("hg", hg_h, hg_v)
    load("res", res_h, res_v)
    load("ng", ng_h, ng_v)

    bar = pltpu.get_barrier_semaphore()
    pals = (
        [{"z": zz(d)} for d in range(1, NZ)]
        + [{"x": xx(d)} for d in range(1, NX)]
        + [{"y": yy(d)} for d in range(1, NY)]
        + [{"c": oc}]
    )
    for pal in pals:
        pl.semaphore_signal(bar, inc=1, device_id=pal, device_id_type=MESH)
    with jax.named_scope("barrier"):
        pl.semaphore_wait(bar, len(pals))

    numbers = {}
    leaving = {}

    def number(key):
        return numbers.setdefault(key, len(numbers))

    def copy(src, dst, n_send, n_recv, dev):
        return pltpu.make_async_remote_copy(
            src_ref=src, dst_ref=dst, send_sem=ssem.at[n_send], recv_sem=rsem.at[n_recv],
            device_id=dev, device_id_type=MESH,
        )

    def send(out, key, src, dst, dev):
        n = leaving.setdefault(out, len(leaving))
        copy(src, dst, n, number(key), dev).start()

    def recv(key, land):
        copy(land, land, 0, number(key), partner).wait_recv()

    def drain(out, like):
        copy(like, like, leaving[out], 0, partner).wait_send()

    right_z, left_z = {"z": zz(1)}, {"z": zz(-1)}
    right_x, left_x = {"x": xx(1)}, {"x": xx(-1)}
    right_y, left_y = {"y": yy(1)}, {"y": yy(-1)}
    partner = {"c": oc}

    def gu(zb, xb, which=None):
        if which is None:
            return wgu.at[zb, xb, c]
        return wgu.at[zb, xb, c, :, pl.ds(which * FFL, FFL)]

    def dn_half(h):
        return pl.ds(0, 768) if h == 0 else pl.ds(768, 640)

    def dnx(xb, h=None):
        if h is None:
            return wdn.at[z, xb, c]
        return wdn.at[z, xb, c, :, dn_half(h)]

    def dnz(zb, h=None):
        if h is None:
            return wdn.at[zb, :, c]
        return wdn.at[zb, :, c, :, dn_half(h)]

    def bz_send(s):
        w0, w1 = (None, None) if s < 4 else (0, 1)
        out = "bz" if s < 4 else "hz"
        send(out, ("bz", s), gu(zz(1 - s), x, w0), gu(zz(1 - s), x, w0), right_z)
        send(out, ("bz", s), gu(zz(s - 1), x, w1), gu(zz(s - 1), x, w1), left_z)

    def bz_recv(s):
        recv(("bz", s), wgu.at[z, 0] if s < 4 else gu(zz(4), x))

    def bz_step(s):
        bz_recv(s)
        if s < 4:
            bz_send(s + 1)

    def bx_send(o):
        send("bx", ("bx", o), gu(zz(o), x), gu(zz(o), x), right_x)
        send("bx", ("bx", o), gu(zz(o), x), gu(zz(o), x), left_x)

    def db_class(o):
        return ("db", max(abs(o), 2))

    def cross(o, d):
        send("db", db_class(o), gu(zz(o), xx(d)), gu(zz(o), xx(d)), partner)

    def bx_mid(o):
        recv(("bx", o), wgu.at[zz(o), 0])
        send("hx", ("hx", o), gu(zz(o), xx(-1), 0), gu(zz(o), xx(-1), 0), right_x)
        send("hx", ("hx", o), gu(zz(o), xx(1), 1), gu(zz(o), xx(1), 1), left_x)
        if abs(o) > 2:
            for d in (0, -1, 1):
                cross(o, d)

    def bx_fin(o):
        recv(("hx", o), gu(zz(o), xx(2)))
        if abs(o) > 2:
            cross(o, 2)
        else:
            send("db", db_class(o), wgu.at[zz(o), :, c], wgu.at[zz(o), :, c], partner)

    def ax_send():
        send("hz", "ax", dnx(x), dnx(x), right_x)
        send("hz", "ax", dnx(x), dnx(x), left_x)

    def ax_mid():
        recv("ax", wdn.at[z, 0])
        send("ax", "hax", dnx(xx(-1), 0), dnx(xx(-1), 0), right_x)
        send("ax", "hax", dnx(xx(1), 1), dnx(xx(1), 1), left_x)

    def ax_fin():
        recv("hax", dnx(xx(2)))

    def az_send(s, h):
        if s < 4:
            send("az", ("az", s, h), dnz(zz(1 - s), h), dnz(zz(1 - s), h), right_z)
            send("az", ("az", s, h), dnz(zz(s - 1), h), dnz(zz(s - 1), h), left_z)
        elif h == 0:
            send("haz", ("az", 4), dnz(zz(-3), 0), dnz(zz(-3), 0), right_z)
        else:
            send("haz", ("az", 4), dnz(zz(3), 1), dnz(zz(3), 1), left_z)

    def az_half(s, h):
        recv(("az", s, h), wdn.at[z, :, :, :, dn_half(h)])
        az_send(s + 1, h)
        if h == 1:
            da_send(-s)
            da_send(s)

    def az_last():
        recv(("az", 4), dnz(zz(4)))
        da_send(4)

    def da_send(o):
        send("da", ("da", o), wdn.at[zz(o), :, c], wdn.at[zz(o), :, c], partner)

    def turn(o):
        recv(("da", o), wdn.at[zz(o), :, oc])
        cols = pl.ds(pl.multiple_of(256 * zz(o), 256), 256)

        @pl.loop(0, FFL // 128, unroll=True)
        def _(n):
            rows = pl.ds(pl.multiple_of(n * 128, 128), 128)
            wdt[rows, cols] = wdn[zz(o), :, :, :, rows].reshape(256, 128).T

    left_cols = pl.ds(0, CL)

    def wo_half(yb, cc):
        return wo.at[yb, pl.ds(pl.multiple_of(256 * cc, 256), 256), left_cols]

    def wo_piece(yb, cc, k):
        return wo.at[yb, pl.ds(pl.multiple_of(256 * cc + 64 * k, 64), 64), left_cols]

    def wo_rows(n):
        return wo.at[y, 0:n, left_cols]

    def wo_quarter(yb, k):
        return wo.at[yb, pl.ds(pl.multiple_of(256 * c + 128 * k, 128), 128), left_cols]

    def wo_send():
        for k in (0, 1):
            send("wo", ("wo", k), wo_quarter(y, k), wo_quarter(y, k), right_y)
            send("wo", ("wo", k), wo_quarter(y, 1 - k), wo_quarter(y, 1 - k), left_y)

    def wo_mid():
        recv(("wo", 0), wo_rows(256))
        for k in (0, 1):
            send("fwo", ("fwo", k), wo_piece(yy(-1), c, k), wo_piece(yy(-1), c, k), right_y)
            send("fwo", ("fwo", k), wo_piece(yy(1), c, 2 + k), wo_piece(yy(1), c, 2 + k), left_y)

    def wo_near():
        recv(("wo", 1), wo_rows(256))
        send("dwo", "dwo", wo_half(yy(-1), c), wo_half(yy(-1), c), partner)
        send("dwo", "dwo", wo_half(yy(1), c), wo_half(yy(1), c), partner)

    def wo_fin():
        for k in (0, 1):
            recv(("fwo", k), wo_rows(128))
            for h in (k, 2 + k):
                send("dfwo", "dfwo", wo_piece(yy(2), c, h), wo_piece(yy(2), c, h), partner)

    local["wg"].wait()
    local["wu"].wait()
    bz_send(1)
    bx_send(0)
    local["wo"].wait()
    wo_send()

    for name in ("fg", "ed", "ig", "k", "v"):
        local[name].wait()
    lane = lax.broadcasted_iota(jnp.int32, (128, 128), 1)
    subl = lax.broadcasted_iota(jnp.int32, (128, 128), 0)
    row8 = lax.broadcasted_iota(jnp.int32, (8, 128), 0)
    low = lane < 64
    causal = subl >= lane

    def by_block(ref):
        return jnp.concatenate(
            [ref[:, 128 * b : 128 * b + 128] for b in range(NB) for _ in (0, 1)], axis=0
        )

    with jax.named_scope("gates"):
        fg, ig, ed = by_block(fg_v), by_block(ig_v), by_block(ed_v)
        wide = (8 * NB, 128)
        lf = jnp.minimum(fg, 0.0) - jnp.log1p(jnp.exp(-jnp.abs(fg))) + ed
        run = lane_scan(lf, jnp.add, 0.0)
        last = lax.broadcasted_iota(jnp.int32, wide, 1) == 127
        tot = jnp.broadcast_to(jnp.sum(jnp.where(last, run, 0.0), axis=1, keepdims=True), wide)
        a = ig - run
        te = tot - run + ig
        bt = jnp.broadcast_to(jnp.max(te, axis=1, keepdims=True), wide)
        fac = jnp.exp(te - bt) * DQK ** (-0.5)
        cm = lane_scan(a, jnp.maximum, -3e38)
        ltop, ltot = jnp.full((8, 128), LOWEST, F32), jnp.zeros((8, 128), F32)
        for b in range(NB):
            at = slice(8 * b, 8 * b + 8)
            ltop_s[b], ltot_s[b] = ltop, ltot
            a_s[b] = a[at]
            ml_s[b] = jnp.maximum(ltop, cm[at])
            fac_s[b] = fac[at]
            top = jnp.maximum(tot[at] + ltop, bt[at])
            e1_s[b] = jnp.exp(tot[at] + ltop - top)
            e2_s[b] = jnp.exp(bt[at] - top)
            ltop, ltot = top, ltot + tot[at]
    lst[...] = jnp.zeros((2, 128, 128), F32)

    with jax.named_scope("states"):
        @pl.loop(0, NB, unroll=True)
        def _(b):
            rows = pl.ds(pl.multiple_of(b * 128, 128), 128)
            fact = fac_s[b].T
            e1, e2 = e1_s[b], e2_s[b]
            for p in (0, 1):
                f2 = jnp.where(low, fact[:, 2 * p : 2 * p + 1], fact[:, 2 * p + 1 : 2 * p + 2])
                wk = (k_v[rows, 128 * p : 128 * p + 128].astype(F32) * f2).astype(BF)
                s2 = tn_dot(wk, v_v[rows, 256 * p : 256 * p + 256])
                sb = jnp.concatenate([s2[0:64, 0:128], s2[64:128, 128:256]], axis=0)
                old = lst[p]
                lpre[b, p] = old.astype(BF)
                lst[p] = expand(e1, 2 * p) * old + expand(e2, 2 * p) * sb

    pack(sm1, 0, (lst[0], ltop, ltot))
    pack(sm1, 1, (lst[1], pltpu.roll(ltop, 6, 0), pltpu.roll(ltot, 6, 0)))
    send("sc", "sc1", sm1.at[oc], cb.at[c], partner)
    cb[c] = sm1[c]

    def inner(b):
        rows = pl.ds(pl.multiple_of(b * 128, 128), 128)
        a, ml = a_s[b], ml_s[b]
        mc = ml.T
        ec = jnp.exp(ltop_s[b] - ml).T
        for p in (0, 1):
            qp = q_v[rows, 128 * p : 128 * p + 128]
            kp = k_v[rows, 128 * p : 128 * p + 128]
            lp = lpre[b, p]
            for e in (0, 1):
                h = 2 * p + e
                qm = jnp.where(low if e == 0 else jnp.logical_not(low), qp, jnp.zeros_like(qp))
                s = nt_dot(qm, kp) * DQK ** (-0.5)
                w = jnp.exp(jnp.where(causal, a[h : h + 1, :] - mc[:, h : h + 1], LOWEST))
                w = (s * w).astype(BF)
                hs = pl.ds(128 * h, 128)
                num[rows, hs] = dot(w, v_v[rows, hs]) + ec[:, h : h + 1] * dot(qm, lp)

    local["q"].wait()
    with jax.named_scope("sc1"):
        recv("sc1", cb.at[oc])
    core0 = unpack(cb, 0)
    pack(xb, x, merge(core0, unpack(cb, 1)))
    for d in (1, 3, 2):
        send("sx", "sx", xb.at[x], xb.at[x], {"x": xx(d)})
    local["wd"].wait()
    ax_send()
    with jax.named_scope("bz1"):
        bz_step(1)
    bx_send(-1)
    bx_send(1)

    with jax.named_scope("inner"):
        @pl.loop(0, NB)
        def _(b):
            inner(b)

    with jax.named_scope("sx"):
        recv("sx", xb.at[0:3])

    def into(ref):
        return lambda k, acc: merge(acc, unpack(ref, k))

    with jax.named_scope("sxmerge"):
        xpre = lax.fori_loop(0, x, into(xb), blank_parts())
        pack(zb, z, lax.fori_loop(x, NX, into(xb), xpre))
    for d in (1, 7, 2, 6, 3, 5, 4):
        send("sz", "sz", zb.at[z], zb.at[z], {"z": zz(d)})
    with jax.named_scope("bxm0"):
        bx_mid(0)
    with jax.named_scope("axm"):
        ax_mid()
    with jax.named_scope("wo_mid"):
        wo_mid()
    with jax.named_scope("bz2"):
        bz_recv(2)
    bx_send(-2)
    bx_send(2)
    with jax.named_scope("sz"):
        recv("sz", zb.at[0:7])
    with jax.named_scope("szmerge"):
        zpre = lax.fori_loop(0, z, into(zb), blank_parts())
        in0 = merge(zpre, xpre)
        pack(st2, 0, in0)
        pack(st2, 1, merge(in0, core0))
    send("sc", "sc2", st2.at[oc], inb.at[c], partner)
    inb[c] = st2[c]
    bz_send(3)
    local["o"].wait()
    local["hg"].wait()
    with jax.named_scope("sc2"):
        recv("sc2", inb.at[oc])
    ta = unpack(inb, 0)[1]
    tb = unpack(inb, 1)[1]
    top_in = jnp.where(row8 < 2, ta, pltpu.roll(tb, 2, 0))

    with jax.named_scope("ecol"):
        for b in range(NB):
            ml = ml_s[b]
            g = ltot_s[b] + top_in
            m = jnp.maximum(ml, g)
            rows = pl.ds(128 * b, 128)
            e1c[rows, :] = jnp.exp(ml - m).T
            e2c[rows, :] = jnp.exp(g - m).T

    low160 = lax.broadcasted_iota(jnp.int32, (MINE, 128), 1) < 64

    def rows_of(d):
        return pl.ds(pl.multiple_of(MINE * yy(d), 32), MINE)

    def finish(d):
        rows = rows_of(d)
        e1, e2 = e1c[rows, :], e2c[rows, :]
        for p in (0, 1):
            qp = q_v[rows, 128 * p : 128 * p + 128]
            sin = inb[p, 0:128, :]
            for e in (0, 1):
                h = 2 * p + e
                hs = pl.ds(128 * h, 128)
                qm = jnp.where(low160 if e == 0 else jnp.logical_not(low160), qp, jnp.zeros_like(qp))
                n = e1[:, h : h + 1] * num[rows, hs] + e2[:, h : h + 1] * dot(qm, sin)
                r = lax.rsqrt(jnp.mean(n * n, axis=1, keepdims=True) + EPS)
                gate = 1.0 / (1.0 + jnp.exp(-o_v[rows, hs].astype(F32)))
                cell[rows, hs] = (n * r * hg_v[:, hs] * gate).astype(BF)

    ha, hb = pl.ds(0, 80), pl.ds(80, 80)

    def half_of(d, h):
        return pl.ds(pl.multiple_of(MINE * yy(d) + 80 * h, 16), 80)

    right_cols, ca_cols, cb_cols = pl.ds(CL, CR), pl.ds(0, CA), pl.ds(CA, CB)

    def share(d):
        po[d - 1] = dot(cell[rows_of(d), :], wo[y, :, right_cols]).astype(BF)

    with jax.named_scope("finish"):
        finish(2)
        share(2)
        send("of", "of", po.at[1, :, ca_cols], ofa, right_y)
        send("of", "of", po.at[1, :, cb_cols], ofb, left_y)
        send("caf", "caf", cell.at[half_of(2, 0)], relay.at[0], right_y)
        send("caf", "caf", cell.at[half_of(2, 1)], relay.at[1], left_y)
        ax_fin()
        az_send(1, 0)
        az_send(1, 1)
        da_send(0)
        finish(1)
        send("ca", "ca", cell.at[rows_of(1)], crows.at[1], right_y)
        finish(3)
        send("ca", "ca", cell.at[rows_of(3)], crows.at[3], left_y)
        share(1)
        send("on", "on", po.at[0, :, cb_cols], on.at[0, :, cb_cols], right_y)
        share(3)
        send("on", "on", po.at[2, :, ca_cols], on.at[1, :, ca_cols], left_y)
    with jax.named_scope("wo_near"):
        wo_near()
    with jax.named_scope("bxm1"):
        bx_mid(-1)
        bx_mid(1)
    with jax.named_scope("finish0"):
        finish(0)

    local["res"].wait()
    local["ng"].wait()

    def project(lhs, yb, first):
        for at, size in ((0, 512), (512, 512), (1024, 256)):
            cols = pl.ds(at, size)
            old = res_v[:, cols].astype(F32) if first else acc[:, cols]
            acc[:, cols] = old + dot(lhs(), wo[yb, :, cols])

    with jax.named_scope("proj0"):
        project(lambda: cell[rows_of(0), :], y, True)
        acc[:, right_cols] = res_v[:, right_cols].astype(F32) + dot(
            cell[rows_of(0), :], wo[y, :, right_cols]
        )
    with jax.named_scope("bz3"):
        bz_step(3)
    bx_send(-3)
    bx_send(3)
    with jax.named_scope("of"):
        recv("of", on.at[0])
        po[0, :, ca_cols] = (po[0, :, ca_cols].astype(F32) + ofa[...].astype(F32)).astype(BF)
        po[2, :, cb_cols] = (po[2, :, cb_cols].astype(F32) + ofb[...].astype(F32)).astype(BF)
    with jax.named_scope("caf"):
        recv("caf", relay)
        send("cag", "cag", relay.at[0], crows.at[2, ha], right_y)
        send("cag", "cag", relay.at[1], crows.at[2, hb], left_y)
    for k, part_rows in enumerate((ha, hb)):
        send("og", ("og", k), po.at[0, part_rows, ca_cols], on.at[0, part_rows, ca_cols], right_y)
        send("og", ("og", k), po.at[2, part_rows, cb_cols], on.at[1, part_rows, cb_cols], left_y)
    with jax.named_scope("wo_fin"):
        wo_fin()
    with jax.named_scope("az10"):
        az_half(1, 0)
    with jax.named_scope("bxf0"):
        bx_fin(0)
    with jax.named_scope("bxm2"):
        bx_mid(-2)
        bx_mid(2)
    with jax.named_scope("az11"):
        az_half(1, 1)
    with jax.named_scope("bz4"):
        bz_recv(4)
    bx_send(4)
    with jax.named_scope("bxf1"):
        bx_fin(-1)
        bx_fin(1)
    with jax.named_scope("ca"):
        recv("ca", crows.at[0:2])
    with jax.named_scope("dwo"):
        recv("dwo", wo_rows(512))
    with jax.named_scope("projnear"):
        project(lambda: crows[1], yy(-1), False)
        project(lambda: crows[3], yy(1), False)
    with jax.named_scope("cag"):
        recv("cag", crows.at[2])
    with jax.named_scope("dwofar"):
        recv("dfwo", wo_rows(256))
    with jax.named_scope("projfar"):
        project(lambda: crows[2], yy(2), False)
    with jax.named_scope("on"):
        recv("on", on.at[0])
    def norm_rows(first):
        @pl.loop(0, 5, unroll=True)
        def _(r):
            rows = pl.ds(pl.multiple_of(first + r * 16, 16), 16)
            right = acc[rows, right_cols] + on[0, rows, :].astype(F32) + on[1, rows, :].astype(F32)
            mb = jnp.concatenate([acc[rows, left_cols], right], axis=1).astype(BF)
            mix[rows, :] = mb
            m = mb.astype(F32)
            scale = lax.rsqrt(jnp.mean(m * m, axis=1, keepdims=True) + EPS)
            here = pl.ds(pl.multiple_of(r * 16, 16), 16)
            xs[first // 80, here, :] = (m * scale * ng_v[...]).astype(BF)

    with jax.named_scope("norm"):
        for k in (0, 1):
            recv(("og", k), on.at[0, 0:80])
            norm_rows(80 * k)
            send("x", ("x", k), xs.at[k], xs.at[2 + k], right_y)
            send("x", ("x", k), xs.at[k], xs.at[4 + k], left_y)

    lh, rh = pl.ds(0, 1024), pl.ds(1024, 1024)

    def x_forward(k):
        recv(("x", k), xs.at[0:2])
        send("xf", "xfar", xs.at[2 + k, :, lh], xs.at[6 + k, :, lh], right_y)
        send("xf", "xfar", xs.at[4 + k, :, rh], xs.at[6 + k, :, rh], left_y)

    with jax.named_scope("az20"):
        az_half(2, 0)
    with jax.named_scope("az21"):
        az_half(2, 1)
    with jax.named_scope("bxm3"):
        bx_mid(-3)
        bx_mid(3)
    with jax.named_scope("turn0"):
        turn(0)
        turn(-1)
    with jax.named_scope("bxf2"):
        bx_fin(-2)
        bx_fin(2)
    with jax.named_scope("turn1"):
        turn(1)
    with jax.named_scope("az30"):
        az_half(3, 0)
    with jax.named_scope("turnm2"):
        turn(-2)
    with jax.named_scope("bxm4"):
        bx_mid(4)
    with jax.named_scope("turn2"):
        turn(2)
    with jax.named_scope("az31"):
        az_half(3, 1)
    with jax.named_scope("xfwd"):
        x_forward(0)
    with jax.named_scope("turn3"):
        turn(-3)
        turn(3)
    with jax.named_scope("bxf3"):
        bx_fin(-3)
        bx_fin(3)
    with jax.named_scope("bxf4"):
        bx_fin(4)
    with jax.named_scope("db3"):
        recv(("db", 2), wgu.at[0:5, :, 0])
        recv(("db", 3), wgu.at[0])

    def gate_and_up(n):
        gc = pl.ds(pl.multiple_of(n * 128, 128), 128)
        uc = pl.ds(pl.multiple_of(FFL + n * 128, 128), 128)
        return gc, uc

    def stacked(blocks, cols):
        return jnp.concatenate([xs[b, :, cols] for b in blocks], axis=0)

    def group_product(blocks, o, gc, uc):
        w = jnp.concatenate(
            [wgu[zz(o), :, :, :, gc].reshape(256, 128), wgu[zz(o), :, :, :, uc].reshape(256, 128)],
            axis=1,
        )
        return dot(stacked(blocks, pl.ds(pl.multiple_of(256 * zz(o), 256), 256)), w)

    with jax.named_scope("partial"):
        @pl.loop(0, FFL // 128, unroll=True)
        def _(n):
            gc, uc = gate_and_up(n)
            total = group_product((2, 4), 0, gc, uc)
            for o in (-1, 1, -2, 2, -3, 3):
                total = total + group_product((2, 4), o, gc, uc)
            begun[:, pl.ds(pl.multiple_of(n * 256, 256), 256)] = total
    with jax.named_scope("az4"):
        az_last()
    with jax.named_scope("xsecond"):
        x_forward(1)
    with jax.named_scope("db4"):
        recv(("db", 4), wgu.at[0, :, 0])

    def activate(blocks, n, r):
        g, u = r[:, :128], r[:, 128:]
        h = (g / (1.0 + jnp.exp(-g)) * u).astype(BF)
        for i, b in enumerate(blocks):
            hid[80 * b : 80 * b + 80, gate_and_up(n)[0]] = h[80 * i : 80 * i + 80]

    def up(blocks, fast=True):
        @pl.loop(0, FFL // 128, unroll=fast)
        def _(n):
            gc, uc = gate_and_up(n)
            w = jnp.concatenate(
                [wgu[:, :, :, :, gc].reshape(D, 128), wgu[:, :, :, :, uc].reshape(D, 128)], axis=1
            )
            activate(blocks, n, dot(stacked(blocks, pl.ds(0, D)), w))

    def down(slots, lo, hi, fast=True):
        first, count = slots

        @pl.loop(lo, hi, unroll=fast)
        def _(n):
            cols = pl.ds(pl.multiple_of(n * 256, 256), 256)
            r = dot(hid[80 * first : 80 * (first + count), :], wdt[:, cols])
            part[first : first + count, :, cols] = r.astype(BF).reshape(count, 80, 256)

    with jax.named_scope("upnear"):
        up((3, 5))

        @pl.loop(0, FFL // 128, unroll=True)
        def _(n):
            done = begun[:, pl.ds(pl.multiple_of(n * 256, 256), 256)]
            activate((2, 4), n, done + group_product((2, 4), 4, *gate_and_up(n)))
    with jax.named_scope("turn4"):
        turn(4)
    with jax.named_scope("dnnear"):
        down((2, 2), 0, 4)
        for k, s in enumerate((2, 3)):
            send("rn", "rn", part.at[s, :, lh], rnear.at[1, k, :, lh], left_y)
        down((4, 2), 4, 8)
        for k, s in enumerate((4, 5)):
            send("rn", "rn", part.at[s, :, rh], rnear.at[0, k, :, rh], right_y)
    with jax.named_scope("xfar"):
        recv("xfar", xs.at[6:8])
    with jax.named_scope("upfar"):
        up((6, 7))
    with jax.named_scope("dnfar"):
        down((6, 2), 0, 4)
        for k in (0, 1):
            send("rf", ("rf", k), part.at[6 + k, :, lh], rfar.at[0, k], right_y)
        down((6, 2), 4, 8)
        for k in (0, 1):
            send("rf", ("rf", k), part.at[6 + k, :, rh], rfar.at[1, k], left_y)
    with jax.named_scope("dnnear2"):
        down((4, 2), 0, 4)
        down((2, 2), 4, 8)
    with jax.named_scope("upown"):
        up((0, 1), False)

    def add_into(slot, half, side, k):
        @pl.loop(0, 5)
        def _(r):
            rows = pl.ds(pl.multiple_of(r * 16, 16), 16)
            part[slot, rows, half] = (
                part[slot, rows, half].astype(F32) + rfar[side, k, rows, :].astype(F32)
            ).astype(BF)

    for k in (0, 1):
        with jax.named_scope("rf%d" % k):
            recv(("rf", k), rfar.at[0])
        after, before = 4 + k, 2 + k
        add_into(after, lh, 0, k)
        send("rg", ("rg", k), part.at[after, :, lh], rnear.at[0, k, :, lh], right_y)
        add_into(before, rh, 1, k)
        send("rg", ("rg", k), part.at[before, :, rh], rnear.at[1, k, :, rh], left_y)
    with jax.named_scope("dnown"):
        down((0, 2), 0, 8, False)
    with jax.named_scope("drain"):
        drain("bz", wgu.at[0, 0:3])
        drain("bx", wgu.at[0:2])
        drain("hx", wdn.at[0:2])
        drain("hz", wdn.at[0, 0:2])
        drain("ax", wdn.at[0, 0, 0])
        drain("az", wdn.at[0:3])
        drain("haz", wdn.at[0, 0:2])
        drain("db", wgu.at[0:4])
        drain("da", wdn.at[0:4])
        drain("wo", wo_rows(512))
        drain("fwo", wo_rows(256))
        drain("dwo", wo_rows(512))
        drain("dfwo", wo_rows(256))
        drain("of", on.at[0])
        drain("on", on.at[0])
        drain("og", on.at[0])
        drain("sc", st2)
        drain("sx", xb.at[0:3])
        drain("sz", zb.at[0:7])
        drain("ca", crows.at[0:2])
        drain("caf", relay)
        drain("cag", relay)
        drain("x", xs.at[0:4])
        drain("xf", xs.at[0:2])
        drain("rn", rfar)
        drain("rf", rfar)

    with jax.named_scope("rn"):
        recv("rn", rfar)
    for k in (0, 1):
        with jax.named_scope("rg%d" % k):
            recv(("rg", k), rfar.at[0])

        @pl.loop(0, 5)
        def _(r):
            rows = pl.ds(pl.multiple_of(r * 16, 16), 16)
            all_rows = pl.ds(pl.multiple_of(80 * k + r * 16, 16), 16)
            t = part[k, rows, :].astype(F32) + rnear[0, k, rows, :].astype(F32)
            t = t + rnear[1, k, rows, :].astype(F32)
            out_v[all_rows, :] = (mix[all_rows, :].astype(F32) + t).astype(BF)

        if k == 0:
            early = pltpu.make_async_copy(out_v.at[ha], out_h.at[ha], lsem.at[0])
            early.start()

    done = pltpu.make_async_copy(out_v.at[hb], out_h.at[hb], lsem.at[1])
    done.start()
    drain("rg", rfar)
    early.wait()
    done.wait()


def per_device(q, k, v, o, ig, fg, ed, hg, res, wo, ng, wg, wu, wd):
    hbm = pl.BlockSpec(memory_space=pltpu.HBM)
    vm = pltpu.VMEM
    scratch = [
        vm((ROWS, 256), BF), vm((ROWS, 256), BF), vm((ROWS, 512), BF), vm((ROWS, 512), BF),
        vm((4, ROWS), F32), vm((4, ROWS), F32), vm((4, ROWS), F32),
        vm((1, 512), F32), vm((MINE, D), BF), vm((1, D), F32),
        vm((NZ, NX, NC, SHARD, 2 * FFL), BF), vm((NZ, NX, NC, SHARD, FFL), BF),
        vm((FFL, D), BF), vm((MINE, 2 * FFL), F32),
        vm((NY, 512, D), BF), vm((8, 80, D), BF), vm((ROWS, FFL), BF),
        vm((8, 80, D), BF), vm((2, 2, 80, 1024), BF), vm((2, 2, 80, D), BF),
        vm((NY, MINE, 512), BF), vm((2, 80, 512), BF),
        vm((3, MINE, CR), BF), vm((MINE, CA), BF), vm((MINE, CB), BF), vm((2, MINE, CR), BF),
        vm((ROWS, 512), BF), vm((ROWS, 512), F32),
        vm((MINE, D), BF), vm((MINE, D), BF),
        vm((NB, 8, 128), F32), vm((NB, 8, 128), F32), vm((NB, 8, 128), F32), vm((NB, 8, 128), F32),
        vm((NB, 8, 128), F32), vm((NB, 8, 128), F32), vm((NB, 8, 128), F32),
        vm((ROWS, 8), F32), vm((ROWS, 8), F32), vm((MINE, D), F32),
        vm((2, 128, 128), F32), vm((NB, 2, 128, 128), BF),
        vm((2, MSG, 128), BF), vm((2, MSG, 128), BF), vm((NX, MSG, 128), BF),
        vm((NZ, MSG, 128), BF), vm((2, MSG, 128), BF), vm((2, MSG, 128), BF),
        pltpu.SemaphoreType.DMA((14,)),
        pltpu.SemaphoreType.DMA((27,)),
        pltpu.SemaphoreType.DMA((65,)),
    ]
    return pl.pallas_call(
        kernel,
        out_shape=jax.ShapeDtypeStruct((MINE, D), BF),
        in_specs=[hbm] * 14,
        out_specs=hbm,
        scratch_shapes=scratch,
        compiler_params=pltpu.CompilerParams(
            collective_id=0, has_side_effects=True, vmem_limit_bytes=60 * 1024 * 1024
        ),
        name="cell_ffn",
    )(q, k, v, o, ig, fg, ed, hg.reshape(1, 512), res, wo, ng.reshape(1, D), wg, wu, wd.T)


def solution(mesh):
    torus = Mesh(mesh.devices.reshape(NZ, NX, NC, NY), SP_TP)
    placed = (
        P(SP, "y"), P(SP, "y"), P(SP, "y"), P(SP, "y"),
        P("y", SP), P("y", SP), P("y", SP),
        P("y"), P(SP_TP, None), P("y", None), P(),
        P(SP, "y"), P(SP, "y"), P("y", SP),
    )
    return jax.shard_map(
        per_device, mesh=torus, in_specs=placed, out_specs=P(SP_TP, None), check_vma=False
    )
```
